32 devices in a mesh: sp: 8 (over z, y), tp: 4 (over x, core).
Axes of the slice: x: 2, y: 2, z: 4, core: 2. Of those that a mesh axis runs over, the one named last changes fastest.
Arguments:
- out_cotangent: bfloat16 [1024, 2048], P('sp', 'tp'), may hold values from -6 to 6
- expert_input: bfloat16 [1024, 2048], P('sp', 'tp'), may hold values from -6 to 6
- routes: int32 [1024, 2], P('sp'), may hold values from 0 to 7, as said below
- route_weights: float32 [1024, 2], P('sp'), may hold values from 0.2 to 1
- gate_proj: bfloat16 [8, 2048, 3584], P('sp', None, 'tp'), may hold values from -0.125 to 0.125
- up_proj: bfloat16 [8, 2048, 3584], P('sp', None, 'tp'), may hold values from -0.125 to 0.125
- down_proj: bfloat16 [8, 3584, 2048], P('sp', 'tp'), may hold values from -0.09375 to 0.09375
- conv_out: bfloat16 [1024, 2048], P('sp', 'tp'), may hold values from -27 to 27
- conv_mean: float32 [1024], P('sp'), may hold values from -3 to 3
- conv_rstd: float32 [1024], P('sp'), may hold values from 0.25 to 1
- norm_gain: float32 [2048], P('tp'), may hold values from 0.1 to 1.9
- taps: float32 [31, 2048], P(None, 'tp'), may hold values from -1 to 1
- out_proj: bfloat16 [2048, 2048], P(None, 'tp'), may hold values from -0.125 to 0.125
Outputs:
- gate_grad: bfloat16 [8, 2048, 3584], P('sp', None, 'tp')
- up_grad: bfloat16 [8, 2048, 3584], P('sp', None, 'tp')
- down_grad: bfloat16 [8, 3584, 2048], P('sp', 'tp')
- proj_grad: float32 [2048, 2048], P('sp', 'tp')
- stream_grad: bfloat16 [1024, 2048], P('sp', 'tp')
- conv_in_grad: bfloat16 [1024, 2048], P('sp', 'tp')
The draws below stay inside these ranges and needn't reach their ends.
Inputs may be any that keep to these rules, and one draw needn't show every extreme that they name: `routes`: each row names 2 different experts. In each aligned block of 128 rows (the rows of one device) no expert is named by more than 48 rows, and one expert, the same in every block, is named by exactly 48 rows of every block.
All inputs are finite; a program needn't handle non-finite values.
Results may differ from the reference program's by a relative error of at most 0.02.
Values may be sent and summed in bfloat16 or wider, within the bound.
A program may use at most 128 MiB of HBM per device.

```python
import math
import jax
import jax.numpy as jnp
from jax import lax

D = 2048
FF = 3584
TOP = 2
TAPS = 31
TOK_DEV = 128
EXPERTS = 8
CAP = 48
TOKENS = 1024
HID_BLOCKS = 4


def draw_routes(key, part):
    blocks = TOKENS // TOK_DEV
    hot_key, rest_key = jax.random.split(jax.random.fold_in(key, 11))
    hottest = jax.random.randint(hot_key, (), 0, EXPERTS).astype(jnp.int32)
    block_keys = jax.random.split(rest_key, blocks)
    spare = 2 * TOK_DEV - CAP
    base_count = spare // (EXPERTS - 1)
    extra_count = spare % (EXPERTS - 1)
    shift_reach = min(base_count, CAP - base_count - 1)
    pair_count = (EXPERTS - 1) // 2

    def one_block(block_key):
        perm_key, shift_key, row_key, side_key = jax.random.split(block_key, 4)
        others = jax.random.permutation(perm_key, EXPERTS - 1).astype(jnp.int32)
        others = others + (others >= hottest).astype(jnp.int32)
        expert_order = jnp.concatenate([hottest[None], others])
        counts = base_count + (jnp.arange(EXPERTS - 1) < extra_count).astype(jnp.int32)
        moves = jax.random.randint(shift_key, (pair_count,), 0, shift_reach + 1).astype(jnp.int32)
        change = jnp.concatenate([jnp.stack([moves, -moves], axis=1).reshape(-1), jnp.zeros((EXPERTS - 1 - 2 * pair_count,), jnp.int32)])
        counts = jnp.concatenate([jnp.full((1,), CAP, jnp.int32), counts + change])
        run_ends = jnp.cumsum(counts)
        position = jnp.arange(2 * TOK_DEV, dtype=jnp.int32)
        run_index = jnp.sum((position[:, None] >= run_ends[None, :]).astype(jnp.int32), axis=1)
        labels = expert_order[run_index]
        first_half = labels[:TOK_DEV]
        second_half = labels[TOK_DEV:]
        row_order = jax.random.permutation(row_key, TOK_DEV)
        flipped = jax.random.randint(side_key, (TOK_DEV,), 0, 2)
        left_col = jnp.where(flipped == 1, second_half, first_half)[row_order]
        right_col = jnp.where(flipped == 1, first_half, second_half)[row_order]
        return jnp.stack([left_col, right_col], axis=1)
    return jax.vmap(one_block)(block_keys).reshape(TOKENS, TOP).astype(jnp.int32)


def draw_conv_out(key, part):
    noise_key, rough_key = jax.random.split(jax.random.fold_in(key, 23))
    channel = jnp.arange(D, dtype=jnp.float32)
    rising = jnp.exp(jnp.log(3.0) * channel / (D - 1))
    rough = jax.random.uniform(rough_key, (D,), jnp.float32, 0.6, 1.5)
    values = jnp.clip(jax.random.normal(noise_key, (TOKENS, D), jnp.float32), -6.0, 6.0)
    return (values * rising[None, :] * rough[None, :]).astype(jnp.bfloat16)


def spiked(result, stream_key, source, target, shards_of, factor):
    owner, partner = [(jnp.arange(result.shape[dim]) // (result.shape[dim] // shards_of)).reshape([-1 if axis == dim else 1 for axis in range(result.ndim)]) for dim in (source, target)]
    chosen = jax.random.permutation(stream_key, shards_of)[partner]
    strong = (owner == chosen) | (owner == (partner + shards_of // 2) % shards_of)
    return jnp.where(strong, factor * result, result)


def levels(own_key, extent, pieces, smallest, largest):
    loudness, own = 1.0, jax.random.fold_in(own_key, 6)
    for axis_at, blocks in pieces:
        draws = jnp.exp(jax.random.uniform(jax.random.fold_in(own, axis_at), (blocks,), jnp.float32, smallest / len(pieces), largest / len(pieces)))
        loudness = loudness * jnp.repeat(draws, extent[axis_at] // blocks).reshape([-1 if axis == axis_at else 1 for axis in range(len(extent))])
    return loudness


def scatter_about(key, dims, deviation, bound, shards=(), kind=jnp.bfloat16):
    level = levels(key, dims, shards, -0.22, 0.18) if shards else 1.0
    drawn = jax.random.normal(key, dims, jnp.float32) * deviation * level
    return jnp.minimum(jnp.maximum(drawn, -bound), bound).astype(kind)


def noise_with(rng, dims, width, bound, cuts, heavy, kind=jnp.bfloat16):
    values = width * jax.random.normal(rng, dims, jnp.float32)
    if cuts:
        values = values * levels(rng, dims, cuts, -0.22, 0.18)
    return jnp.clip(spiked(values, jax.random.fold_in(rng, 3), *heavy), -bound, bound).astype(kind)


def setup_inputs(seed: int = 0) -> dict:
    splits = jax.random.split(jax.random.key(seed), 14)
    return {
        "out_cotangent": noise_with(splits[0], (TOKENS, D), 1.0, 6.0, ((0, 8), (1, 4)), (0, 1, 8, 2.0)),
        "expert_input": scatter_about(splits[1], (TOKENS, D), 1.0, 6.0, ((0, 8), (1, 4))),
        "routes": draw_routes(jax.random.fold_in(splits[13], 71), 0),
        "route_weights": jnp.clip(0.2 + 0.8 * jax.random.uniform(splits[3], (TOKENS, TOP), jnp.float32) ** levels(splits[3], (TOKENS, TOP), ((0, 8),), -0.2, 0.2), 0.2, 1.0),
        "gate_proj": scatter_about(splits[4], (EXPERTS, D, FF), D ** -0.5, 0.125, ((0, 8), (2, 4))),
        "up_proj": scatter_about(splits[5], (EXPERTS, D, FF), D ** -0.5, 0.125, ((0, 8), (2, 4))),
        "down_proj": scatter_about(splits[6], (EXPERTS, FF, D), FF ** -0.5, 0.09375, ((0, 8), (1, 4))),
        "conv_out": draw_conv_out(jax.random.fold_in(splits[13], 71), 0),
        "conv_mean": scatter_about(splits[8], (TOKENS,), 0.5, 3.0, ((0, 8),), jnp.float32),
        "conv_rstd": jnp.clip(jnp.exp(math.log(1.0) - 1.3862944 * jax.random.uniform(splits[9], (TOKENS,), jnp.float32) ** levels(splits[9], (TOKENS,), ((0, 8),), -0.2, 0.2)), 0.25, 1.0),
        "norm_gain": jnp.clip(1.0 + 0.18 * jax.random.normal(splits[10], (D,), jnp.float32), 0.1, 1.9),
        "taps": scatter_about(splits[11], (TAPS, D), TAPS ** -0.5, 1.0, ((1, 4),), jnp.float32),
        "out_proj": scatter_about(splits[12], (D, D), D ** -0.5, 0.125, ((1, 4),)),
    }


OUTER_DIMS = (((0,), (0,)), ((), ()))
INNER_DIMS = (((1,), (1,)), ((), ()))


def reference(out_cotangent, expert_input, routes, route_weights, gate_proj, up_proj, down_proj, conv_out, conv_mean, conv_rstd, norm_gain, taps, out_proj):
    assigned = routes.reshape(-1).astype(jnp.int32)
    pair_weights = route_weights.reshape(-1)
    limit = CAP * EXPERTS
    outside = TOKENS * TOP
    block_width = FF // HID_BLOCKS

    def one_expert(expert_id):
        picked = jnp.nonzero(assigned == expert_id, size=limit, fill_value=outside)[0].astype(jnp.int32)
        usable = picked < outside
        safe_pair = jnp.where(usable, picked, 0)
        token_index = safe_pair // TOP
        rows = jnp.where(usable[:, None], expert_input[token_index], jnp.zeros((), jnp.bfloat16))
        weight = jnp.where(usable, pair_weights[safe_pair], 0.0)
        routed_cot = (weight[:, None] * out_cotangent[token_index].astype(jnp.float32)).astype(jnp.bfloat16)
        gate_local = gate_proj[expert_id]
        up_local = up_proj[expert_id]
        down_local = down_proj[expert_id]
        gate_pre = jnp.dot(rows, gate_local, preferred_element_type=jnp.float32)
        up_pre = jnp.dot(rows, up_local, preferred_element_type=jnp.float32)
        gate_sigmoid = jax.nn.sigmoid(gate_pre)
        activation = (gate_pre * gate_sigmoid * up_pre).astype(jnp.bfloat16)
        act_grad = lax.dot_general(routed_cot, down_local, INNER_DIMS, preferred_element_type=jnp.float32)
        gate_back = (act_grad * up_pre * gate_sigmoid * (1.0 + gate_pre * (1.0 - gate_sigmoid))).astype(jnp.bfloat16)
        up_back = (act_grad * gate_pre * gate_sigmoid).astype(jnp.bfloat16)
        down_part = lax.dot_general(activation, routed_cot, OUTER_DIMS, preferred_element_type=jnp.float32).astype(jnp.bfloat16)
        gate_part = lax.dot_general(rows, gate_back, OUTER_DIMS, preferred_element_type=jnp.float32).astype(jnp.bfloat16)
        up_part = lax.dot_general(rows, up_back, OUTER_DIMS, preferred_element_type=jnp.float32).astype(jnp.bfloat16)
        block_parts = jnp.einsum('lbu,dbu->lbd', gate_back.astype(jnp.float32).reshape(limit, HID_BLOCKS, block_width), gate_local.astype(jnp.float32).reshape(D, HID_BLOCKS, block_width))
        block_parts = block_parts + jnp.einsum('lbu,dbu->lbd', up_back.astype(jnp.float32).reshape(limit, HID_BLOCKS, block_width), up_local.astype(jnp.float32).reshape(D, HID_BLOCKS, block_width))
        block_parts = block_parts.astype(jnp.bfloat16)
        routed_grad = jnp.sum(block_parts.astype(jnp.float32), axis=1).astype(jnp.bfloat16)
        return gate_part, up_part, down_part, routed_grad, picked

    gate_grad, up_grad, down_grad, routed_grad, picked = lax.map(one_expert, jnp.arange(EXPERTS, dtype=jnp.int32))
    placed = jnp.zeros((outside, D), jnp.bfloat16).at[picked.reshape(-1)].set(routed_grad.reshape(-1, D), mode="drop")
    routed_sum = jnp.sum(placed.reshape(TOKENS, TOP, D).astype(jnp.float32), axis=1)
    stream_grad = (out_cotangent.astype(jnp.float32) + routed_sum).astype(jnp.bfloat16)

    normed = (conv_out.astype(jnp.float32) - conv_mean[:, None]) * conv_rstd[:, None]
    scaled = normed * norm_gain[None, :]
    scaled_sigmoid = jax.nn.sigmoid(scaled)
    swished = (scaled * scaled_sigmoid).astype(jnp.bfloat16)
    proj_grad = lax.dot_general(stream_grad, swished, OUTER_DIMS, preferred_element_type=jnp.float32)
    swished_grad = jnp.dot(stream_grad, out_proj, preferred_element_type=jnp.float32)
    scaled_grad = swished_grad * scaled_sigmoid * (1.0 + scaled * (1.0 - scaled_sigmoid)) * norm_gain[None, :]
    first_mean = jnp.mean(scaled_grad, axis=1, keepdims=True)
    second_mean = jnp.mean(scaled_grad * normed, axis=1, keepdims=True)
    conv_grad = conv_rstd[:, None] * (scaled_grad - first_mean - normed * second_mean)
    padded = jnp.concatenate([conv_grad, jnp.zeros((TAPS - 1, D), jnp.float32)], axis=0)
    conv_sum = jnp.zeros((TOKENS, D), jnp.float32)
    for offset in range(TAPS):
        conv_sum = conv_sum + taps[offset][None, :] * padded[offset:offset + TOKENS]
    return gate_grad, up_grad, down_grad, proj_grad, stream_grad, conv_sum.astype(jnp.bfloat16)
```

```python
import functools

import jax
import jax.numpy as jnp
from jax import lax
from jax.experimental import pallas as pl
from jax.experimental.pallas import tpu as pltpu
from jax.sharding import PartitionSpec as P

OUTER_DIMS = (((0,), (0,)), ((), ()))
INNER_DIMS = (((1,), (1,)), ((), ()))
MESH = pl.DeviceIdType.MESH
VMEM = pltpu.VMEM


def flipped(index, bit):
    return index + bit - 2 * bit * ((index // bit) % 2)


def bits_of(count):
    bits, bit = [], 1
    while bit < count:
        bits.append(bit)
        bit *= 2
    return bits


def greet(devices):
    barrier = pltpu.get_barrier_semaphore()
    for device in devices:
        pl.semaphore_signal(barrier, inc=1, device_id=device, device_id_type=MESH)
    pl.semaphore_wait(barrier, len(devices))


def remote(src, dst, send_sem, recv_sem, device):
    return pltpu.make_async_remote_copy(
        src_ref=src, dst_ref=dst, send_sem=send_sem, recv_sem=recv_sem,
        device_id=device, device_id_type=MESH,
    )


def dispatch_kernel(
    experts, parts, send_ref, swished_ref, full_ref, gathered_ref,
    out_send, out_recv, sw_send, sw_recv, hop_send, hop_recv, local_sem,
):
    me, col = lax.axis_index("sp"), lax.axis_index("tp")
    width = send_ref.shape[3]
    bits = bits_of(parts)[::-1]
    greet(
        [(lax.rem(me + k, experts), col) for k in range(1, experts)]
        + [(me, flipped(col, bit)) for bit in bits]
    )

    def place(source, column):
        return full_ref.at[:, source, :, pl.ds(pl.multiple_of(column * width, width), width)]

    own = pltpu.make_async_copy(send_ref.at[me], place(me, col), local_sem.at[0])
    own.start()
    own_sw = pltpu.make_async_copy(swished_ref, gathered_ref.at[me], local_sem.at[1])
    own_sw.start()

    def out_copy(peer, slot):
        return remote(send_ref.at[peer], place(me, col), out_send.at[peer], out_recv.at[me], (peer, col))

    def sw_copy(peer):
        return remote(swished_ref, gathered_ref.at[me], sw_send.at[peer], sw_recv.at[me], (peer, col))

    def start_out(k, carry):
        out_copy(lax.rem(me + k, experts), k).start()
        return carry

    def start_sw(k, carry):
        sw_copy(lax.rem(me + k, experts)).start()
        return carry

    lax.fori_loop(1, experts, start_out, 0)
    lax.fori_loop(1, experts, start_sw, 0)
    own.wait()

    held = [[col]]
    for bit in bits:
        held.append(held[-1] + [flipped(column, bit) for column in held[-1]])
    starts, total = [], 0
    for level in range(len(bits)):
        starts.append(total)
        total += len(held[level])

    def hop(level, slot, column, source):
        index = starts[level] + slot
        return remote(
            place(source, column), place(source, column),
            hop_send.at[index, source], hop_recv.at[index, source],
            (me, flipped(col, bits[level])),
        )

    def hop_arrival(level, slot, source):
        index = starts[level] + slot
        column = flipped(held[level][slot], bits[level])
        return remote(
            place(source, column), place(source, column),
            hop_send.at[index, source], hop_recv.at[index, source],
            (me, flipped(col, bits[level])),
        )

    def advance(k, carry):
        source = lax.rem(me - k + experts, experts)

        @pl.when((k > 0) & (k < experts))
        def _():
            remote(
                send_ref.at[source], place(source, col), out_send.at[source],
                out_recv.at[source], (source, col),
            ).wait_recv()

        @pl.when(k < experts)
        def _():
            for level in range(len(bits)):
                hop(level, 0, col, source).start()

        for level in range(1, len(bits)):
            late = lax.rem(me - k + level + 2 * experts, experts)

            @pl.when((k >= level) & (k < experts + level))
            def _(level=level, late=late):
                size = len(held[level - 1])
                for slot in range(size):
                    hop_arrival(level - 1, slot, late).wait_recv()
                for later in range(level, len(bits)):
                    for slot in range(size, 2 * size):
                        hop(later, slot, held[level][slot], late).start()

        return carry

    lax.fori_loop(0, experts + len(bits) - 1, advance, 0)

    def finish(k, carry):
        source = lax.rem(me + k, experts)
        last = len(bits) - 1
        for slot in range(len(held[last])):
            hop_arrival(last, slot, source).wait_recv()
        for level in range(len(bits)):
            for slot in range(len(held[level])):
                hop(level, slot, held[level][slot], source).wait_send()

        @pl.when(k > 0)
        def _():
            out_copy(source, k).wait_send()
            sw_copy(source).wait_send()
            remote(
                swished_ref, gathered_ref.at[source], sw_send.at[source],
                sw_recv.at[source], (source, col),
            ).wait_recv()

        return carry

    lax.fori_loop(0, experts, finish, 0)
    own_sw.wait()


def dispatch(send, swished, experts, parts):
    _, _, capacity, width = send.shape
    hops = parts - 1
    return pl.pallas_call(
        functools.partial(dispatch_kernel, experts, parts),
        out_shape=(
            jax.ShapeDtypeStruct((2, experts, capacity, width * parts), jnp.bfloat16),
            jax.ShapeDtypeStruct((experts,) + swished.shape, jnp.bfloat16),
        ),
        in_specs=[pl.BlockSpec(memory_space=VMEM)] * 2,
        out_specs=[pl.BlockSpec(memory_space=VMEM)] * 2,
        scratch_shapes=[pltpu.SemaphoreType.DMA((experts,))] * 4
        + [pltpu.SemaphoreType.DMA((hops, experts))] * 2
        + [pltpu.SemaphoreType.DMA((2,))],
        compiler_params=pltpu.CompilerParams(collective_id=0, has_side_effects=True),
        name="dispatch",
    )(send, swished)


def combine_kernel(
    experts, parts, partial_ref, routed_ref, *rest
):
    bits = bits_of(parts)
    levels = len(bits)
    recv_bufs = rest[:levels]
    work, final = rest[levels], rest[levels + 1]
    hop_send, hop_recv, out_send, out_recv = rest[levels + 2 :]
    me, col = lax.axis_index("sp"), lax.axis_index("tp")
    width = routed_ref.shape[2]
    greet(
        [(lax.rem(me + k, experts), col) for k in range(1, experts)]
        + [(me, flipped(col, bit)) for bit in bits]
    )

    kept = [[col]]
    for bit in reversed(bits):
        kept.insert(0, kept[0] + [flipped(column, bit) for column in kept[0]])
    starts, total = [], 0
    for level in range(levels):
        starts.append(total)
        total += len(kept[level + 1])

    def columns(column):
        return pl.ds(pl.multiple_of(column * width, width), width)

    def hop(level, slot, block):
        column = flipped(kept[level + 1][slot], bits[level])
        index = starts[level] + slot
        if level == 0:
            src = partial_ref.at[block, :, columns(column)]
        else:
            src = work.at[level - 1, slot, block]
        return remote(
            src, recv_bufs[level].at[slot, block], hop_send.at[index, block],
            hop_recv.at[index, block], (me, flipped(col, bits[level])),
        )

    def summed(level, slot_column, slot_path, block):
        value = partial_ref[block, :, columns(slot_column)].astype(jnp.float32)
        for stage in range(level):
            value = value + recv_bufs[stage][slot_path[stage], block].astype(jnp.float32)
        return value

    def block_of(k):
        return lax.rem(me + k, experts)

    def start_first(k, carry):
        for slot in range(len(kept[1])):
            hop(0, slot, block_of(k)).start()
        return carry

    lax.fori_loop(1, experts + 1, start_first, 0)

    for level in range(1, levels):

        def middle(k, carry, level=level):
            block = block_of(k)
            for slot in range(len(kept[level])):
                hop(level - 1, slot, block).wait_recv()
            size = len(kept[level + 1])
            for slot in range(size):
                value = summed(
                    level, kept[level][size + slot], [size + slot] * level, block
                )
                work[level - 1, slot, block] = value.astype(jnp.bfloat16)
            for slot in range(size):
                hop(level, slot, block).start()
            return carry

        lax.fori_loop(1, experts + 1, middle, 0)

    def out_copy(block):
        return remote(
            final.at[block], routed_ref.at[me], out_send.at[block], out_recv.at[me], (block, col)
        )

    def last(k, carry):
        block = block_of(k)
        hop(levels - 1, 0, block).wait_recv()
        value = summed(levels, col, [0] * levels, block).astype(jnp.bfloat16)

        @pl.when(k < experts)
        def _():
            final[block] = value
            out_copy(block).start()

        @pl.when(k == experts)
        def _():
            routed_ref[me] = value

        return carry

    lax.fori_loop(1, experts + 1, last, 0)

    def finish(k, carry):
        block = block_of(k)
        for level in range(levels):
            for slot in range(len(kept[level + 1])):
                hop(level, slot, block).wait_send()

        @pl.when(k < experts)
        def _():
            out_copy(block).wait_send()
            remote(
                final.at[block], routed_ref.at[block], out_send.at[block],
                out_recv.at[block], (block, col),
            ).wait_recv()

        return carry

    lax.fori_loop(1, experts + 1, finish, 0)


def combine(partial, experts, parts):
    _, capacity, full = partial.shape
    width = full // parts
    levels = len(bits_of(parts))
    hops = parts - 1
    recv = [
        VMEM((parts >> (level + 1), experts, capacity, width), jnp.bfloat16)
        for level in range(levels)
    ]
    return pl.pallas_call(
        functools.partial(combine_kernel, experts, parts),
        out_shape=jax.ShapeDtypeStruct((experts, capacity, width), jnp.bfloat16),
        in_specs=[pl.BlockSpec(memory_space=VMEM)],
        out_specs=pl.BlockSpec(memory_space=VMEM),
        scratch_shapes=recv
        + [
            VMEM((max(levels - 1, 1), max(parts // 4, 1), experts, capacity, width), jnp.bfloat16),
            VMEM((experts, capacity, width), jnp.bfloat16),
            pltpu.SemaphoreType.DMA((hops, experts)),
            pltpu.SemaphoreType.DMA((hops, experts)),
            pltpu.SemaphoreType.DMA((experts,)),
            pltpu.SemaphoreType.DMA((experts,)),
        ],
        compiler_params=pltpu.CompilerParams(collective_id=1, has_side_effects=True),
        name="combine",
    )(partial)


def tail_kernel(
    experts, parts, stream_ref, conv_out_ref, mean_ref, rstd_ref, gain_ref, taps_ref, proj_ref,
    gathered_ref, conv_ref, proj_grad_ref,
    whole, arrived, extended, stats, grads, norms,
    hop_send, hop_recv, out_send, out_recv, stat_send, stat_recv, halo_sem, local_sem,
):
    me, col = lax.axis_index("sp"), lax.axis_index("tp")
    width, rows = stream_ref.shape
    full = width * parts
    block = full // experts
    bits = bits_of(parts)[::-1]
    tap_count = taps_ref.shape[0]
    halo = extended.shape[0] - rows
    greet(
        [(lax.rem(me + k, experts), col) for k in range(1, experts)]
        + [(me, lax.rem(col + k, parts)) for k in range(1, parts)]
    )

    def part(column):
        return whole.at[pl.ds(pl.multiple_of(column * width, width), width), :]

    own = pltpu.make_async_copy(stream_ref, part(col), local_sem.at[0])
    own.start()
    index, held, copies = 0, [col], []
    for level, bit in enumerate(bits):
        for slot, column in enumerate(held):
            src = stream_ref if column is col else part(column)
            copy = remote(
                src, part(column), hop_send.at[index + slot], hop_recv.at[index + slot],
                (me, flipped(col, bit)),
            )
            copy.start()
            copies.append(copy)
        for slot in range(len(held)):
            column = flipped(held[slot], bit)
            remote(
                part(column), part(column), hop_send.at[index + slot], hop_recv.at[index + slot],
                (me, flipped(col, bit)),
            ).wait_recv()
        index += len(held)
        held = held + [flipped(column, bit) for column in held]
    own.wait()

    def piece(peer):
        return whole.at[pl.ds(pl.multiple_of(peer * block, block), block), :]

    def landing(source):
        return arrived.at[:, pl.ds(pl.multiple_of(source * rows, rows), rows)]

    def out_copy(peer):
        return remote(piece(peer), landing(me), out_send.at[peer], out_recv.at[me], (peer, col))

    def start_out(k, carry):
        out_copy(lax.rem(me + k, experts)).start()
        return carry

    lax.fori_loop(1, experts, start_out, 0)
    mine = pltpu.make_async_copy(piece(me), landing(me), local_sem.at[1])
    mine.start()

    gain = gain_ref[...]
    rstd = rstd_ref[...]
    swished_grad = lax.dot_general(
        whole[...], proj_ref[...], OUTER_DIMS, preferred_element_type=jnp.float32
    )
    normed = (conv_out_ref[...].astype(jnp.float32) - mean_ref[...]) * rstd
    scaled = normed * gain
    sig = jax.nn.sigmoid(scaled)
    scaled_grad = swished_grad * sig * (1.0 + scaled * (1.0 - sig)) * gain
    grads[...] = scaled_grad
    norms[...] = normed
    first = jnp.sum(scaled_grad, axis=1, keepdims=True)
    second = jnp.sum(scaled_grad * normed, axis=1, keepdims=True)
    lane = lax.broadcasted_iota(jnp.int32, (rows, 128), 1)
    both = jnp.where(lane == 0, first, second)
    stats[parts] = both.T[:8]
    stat_copies = []
    for k in range(1, parts):
        copy = remote(
            stats.at[parts], stats.at[k], stat_send.at[k], stat_recv.at[k],
            (me, lax.rem(col + k, parts)),
        )
        copy.start()
        stat_copies.append(copy)
    for copy in stat_copies:
        copy.wait()
    total = stats[parts]
    for k in range(1, parts):
        total = total + stats[k]
    total = total / full
    spread = jnp.concatenate([total] * 16, axis=0).T
    first_mean = spread[:, 0:1]
    second_mean = spread[:, 1:2]
    extended[0:rows, :] = rstd * (grads[...] - first_mean - norms[...] * second_mean)

    def halo_copy(device):
        return remote(
            extended.at[pl.ds(0, halo), :], extended.at[pl.ds(rows, halo), :],
            halo_sem.at[0], halo_sem.at[1], (device, col),
        )

    @pl.when(me > 0)
    def _():
        halo_copy(lax.rem(me + experts - 1, experts)).start()

    @pl.when(me == experts - 1)
    def _():
        extended[rows:, :] = jnp.zeros((halo, width), jnp.float32)

    @pl.when(me < experts - 1)
    def _():
        halo_copy(lax.rem(me + experts - 1, experts)).wait_recv()

    for start in range(0, width, 128):
        cols = pl.ds(start, 128)
        total = jnp.zeros((rows, 128), jnp.float32)
        for offset in range(tap_count):
            total = total + taps_ref[offset : offset + 1, cols] * extended[pl.ds(offset, rows), cols]
        conv_ref[:, cols] = total.astype(jnp.bfloat16)

    def finish(k, carry):
        source = lax.rem(me - k + experts, experts)
        remote(
            piece(source), landing(source), out_send.at[source], out_recv.at[source], (source, col)
        ).wait_recv()
        out_copy(source).wait_send()
        return carry

    lax.fori_loop(1, experts, finish, 0)
    mine.wait()
    proj_grad_ref[...] = jnp.dot(
        arrived[...], gathered_ref[...], preferred_element_type=jnp.float32
    )
    for copy in copies:
        copy.wait_send()

    @pl.when(me > 0)
    def _():
        halo_copy(lax.rem(me + experts - 1, experts)).wait_send()


def tail(stream_t, conv_out, mean, rstd, gain, taps, proj, gathered, experts, parts):
    width, rows = stream_t.shape
    full = width * parts
    block = full // experts
    halo = -(-(taps.shape[0] - 1) // 8) * 8
    return pl.pallas_call(
        functools.partial(tail_kernel, experts, parts),
        out_shape=(
            jax.ShapeDtypeStruct((rows, width), jnp.bfloat16),
            jax.ShapeDtypeStruct((block, width), jnp.float32),
        ),
        in_specs=[pl.BlockSpec(memory_space=VMEM)] * 8,
        out_specs=[pl.BlockSpec(memory_space=VMEM)] * 2,
        scratch_shapes=[
            VMEM((full, rows), jnp.bfloat16),
            VMEM((block, experts * rows), jnp.bfloat16),
            VMEM((rows + halo, width), jnp.float32),
            VMEM((parts + 1, 8, rows), jnp.float32),
            VMEM((rows, width), jnp.float32),
            VMEM((rows, width), jnp.float32),
            pltpu.SemaphoreType.DMA((parts - 1,)),
            pltpu.SemaphoreType.DMA((parts - 1,)),
            pltpu.SemaphoreType.DMA((experts,)),
            pltpu.SemaphoreType.DMA((experts,)),
            pltpu.SemaphoreType.DMA((parts,)),
            pltpu.SemaphoreType.DMA((parts,)),
            pltpu.SemaphoreType.DMA((2,)),
            pltpu.SemaphoreType.DMA((2,)),
        ],
        compiler_params=pltpu.CompilerParams(collective_id=2, has_side_effects=True),
        name="tail",
    )(stream_t, conv_out, mean, rstd, gain, taps, proj, gathered)


def body(
    out_cotangent,
    expert_input,
    routes,
    route_weights,
    gate_proj,
    up_proj,
    down_proj,
    conv_out,
    conv_mean,
    conv_rstd,
    norm_gain,
    taps,
    out_proj,
):
    tok_rows, local_width = out_cotangent.shape
    experts = lax.axis_size("sp")
    parts = lax.axis_size("tp")
    capacity = 3 * tok_rows // experts
    full_width = local_width * parts
    slots = experts * capacity

    chosen = routes[:, :, None] == jnp.arange(experts, dtype=jnp.int32)[None, None, :]
    named = jnp.any(chosen, axis=1)
    weight = jnp.sum(jnp.where(chosen, route_weights[:, :, None], 0.0), axis=1)
    before = jnp.arange(tok_rows)[None, :] < jnp.arange(tok_rows)[:, None]
    rank = jnp.dot(
        before.astype(jnp.bfloat16), named.astype(jnp.bfloat16), preferred_element_type=jnp.float32
    ).astype(jnp.int32)
    rank = jnp.where(named, rank, -1)
    pick = rank.T[:, None, :] == jnp.arange(capacity, dtype=jnp.int32)[None, :, None]
    slot_weight = jnp.sum(jnp.where(pick, weight.T[:, None, :], 0.0), axis=2)
    pick = pick.astype(jnp.bfloat16).reshape(slots, tok_rows)
    send_rows = jnp.dot(pick, expert_input, preferred_element_type=jnp.float32).astype(jnp.bfloat16)
    send_cot = (
        jnp.dot(pick, out_cotangent, preferred_element_type=jnp.float32)
        * slot_weight.reshape(slots, 1)
    ).astype(jnp.bfloat16)
    send = jnp.stack(
        [send_rows.reshape(experts, capacity, local_width), send_cot.reshape(experts, capacity, local_width)],
        axis=1,
    )
    normed = (conv_out.astype(jnp.float32) - conv_mean[:, None]) * conv_rstd[:, None]
    scaled = normed * norm_gain[None, :]
    swished = (scaled * jax.nn.sigmoid(scaled)).astype(jnp.bfloat16)

    arrived, gathered = dispatch(send, swished, experts, parts)
    rows_in = arrived[0].reshape(slots, full_width)
    cot_in = arrived[1].reshape(slots, full_width)
    gate_local = gate_proj[0]
    up_local = up_proj[0]
    down_local = down_proj[0]
    gate_pre = jnp.dot(rows_in, gate_local, preferred_element_type=jnp.float32)
    up_pre = jnp.dot(rows_in, up_local, preferred_element_type=jnp.float32)
    gate_sigmoid = jax.nn.sigmoid(gate_pre)
    activation = (gate_pre * gate_sigmoid * up_pre).astype(jnp.bfloat16)
    act_grad = lax.dot_general(cot_in, down_local, INNER_DIMS, preferred_element_type=jnp.float32)
    gate_back = (act_grad * up_pre * gate_sigmoid * (1.0 + gate_pre * (1.0 - gate_sigmoid))).astype(
        jnp.bfloat16
    )
    up_back = (act_grad * gate_pre * gate_sigmoid).astype(jnp.bfloat16)
    down_grad = lax.dot_general(
        activation, cot_in, OUTER_DIMS, preferred_element_type=jnp.float32
    ).astype(jnp.bfloat16)[None]
    gate_grad = lax.dot_general(
        rows_in, gate_back, OUTER_DIMS, preferred_element_type=jnp.float32
    ).astype(jnp.bfloat16)[None]
    up_grad = lax.dot_general(
        rows_in, up_back, OUTER_DIMS, preferred_element_type=jnp.float32
    ).astype(jnp.bfloat16)[None]
    partial_rows = lax.dot_general(
        gate_back, gate_local, INNER_DIMS, preferred_element_type=jnp.float32
    )
    partial_rows = partial_rows + lax.dot_general(
        up_back, up_local, INNER_DIMS, preferred_element_type=jnp.float32
    )
    partial = partial_rows.astype(jnp.bfloat16).reshape(experts, capacity, full_width)
    routed = combine(partial, experts, parts).reshape(slots, local_width)
    routed_sum = lax.dot_general(pick, routed, OUTER_DIMS, preferred_element_type=jnp.float32)
    stream = (out_cotangent.astype(jnp.float32) + routed_sum).astype(jnp.bfloat16)
    conv_in_grad, proj_grad = tail(
        stream.T, conv_out, conv_mean[:, None], conv_rstd[:, None], norm_gain[None, :], taps,
        out_proj, gathered.reshape(experts * tok_rows, local_width), experts, parts,
    )
    return (gate_grad, up_grad, down_grad, proj_grad, stream, conv_in_grad)


def solution(mesh):
    in_specs = (
        P("sp", "tp"),
        P("sp", "tp"),
        P("sp", None),
        P("sp", None),
        P("sp", None, "tp"),
        P("sp", None, "tp"),
        P("sp", "tp", None),
        P("sp", "tp"),
        P("sp"),
        P("sp"),
        P("tp"),
        P(None, "tp"),
        P(None, "tp"),
    )
    out_specs = (
        P("sp", None, "tp"),
        P("sp", None, "tp"),
        P("sp", "tp", None),
        P("sp", "tp"),
        P("sp", "tp"),
        P("sp", "tp"),
    )
    return jax.shard_map(body, mesh=mesh, in_specs=in_specs, out_specs=out_specs, check_vma=False)
```

```python
import functools

import jax
import jax.numpy as jnp
from jax import lax
from jax.experimental import pallas as pl
from jax.experimental.pallas import tpu as pltpu
from jax.sharding import PartitionSpec as P

OUTER_DIMS = (((0,), (0,)), ((), ()))
INNER_DIMS = (((1,), (1,)), ((), ()))
MESH = pl.DeviceIdType.MESH
VMEM = pltpu.VMEM


def flipped(index, bit):
    return index + bit - 2 * bit * ((index // bit) % 2)


def bits_of(count):
    bits, bit = [], 1
    while bit < count:
        bits.append(bit)
        bit *= 2
    return bits


def greet(devices):
    barrier = pltpu.get_barrier_semaphore()
    for device in devices:
        pl.semaphore_signal(barrier, inc=1, device_id=device, device_id_type=MESH)
    pl.semaphore_wait(barrier, len(devices))


def remote(src, dst, send_sem, recv_sem, device):
    return pltpu.make_async_remote_copy(
        src_ref=src, dst_ref=dst, send_sem=send_sem, recv_sem=recv_sem,
        device_id=device, device_id_type=MESH,
    )


def dispatch_kernel(
    experts, parts, rows_send_ref, cot_send_ref, rows_ref, cot_ref,
    out_send, out_recv, hop_send, hop_recv, local_sem,
):
    me, col = lax.axis_index("sp"), lax.axis_index("tp")
    width = rows_send_ref.shape[2]
    bits = bits_of(parts)[::-1]
    greet(
        [(lax.rem(me + k, experts), col) for k in range(1, experts)]
        + [(me, flipped(col, bit)) for bit in bits]
    )
    sends, fulls = (rows_send_ref, cot_send_ref), (rows_ref, cot_ref)

    def place(kind, source, column):
        return fulls[kind].at[source, :, pl.ds(pl.multiple_of(column * width, width), width)]

    def out_copy(kind, peer):
        return remote(
            sends[kind].at[peer], place(kind, me, col), out_send.at[kind, peer],
            out_recv.at[kind, me], (peer, col),
        )

    own = []
    for kind in range(2):
        own.append(
            pltpu.make_async_copy(sends[kind].at[me], place(kind, me, col), local_sem.at[kind])
        )
        own[kind].start()

        def start_out(k, carry, kind=kind):
            out_copy(kind, lax.rem(me + k, experts)).start()
            return carry

        lax.fori_loop(1, experts, start_out, 0)
    for copy in own:
        copy.wait()

    held = [[col]]
    for bit in bits:
        held.append(held[-1] + [flipped(column, bit) for column in held[-1]])
    starts, total = [], 0
    for level in range(len(bits)):
        starts.append(total)
        total += len(held[level])

    def hop(kind, level, slot, column, source):
        index = starts[level] + slot
        return remote(
            place(kind, source, column), place(kind, source, column),
            hop_send.at[kind, index, source], hop_recv.at[kind, index, source],
            (me, flipped(col, bits[level])),
        )

    def hop_arrival(kind, level, slot, source):
        return hop(kind, level, slot, flipped(held[level][slot], bits[level]), source)

    for kind in range(2):

        def advance(k, carry, kind=kind):
            source = lax.rem(me - k + experts, experts)

            @pl.when((k > 0) & (k < experts))
            def _():
                remote(
                    sends[kind].at[source], place(kind, source, col), out_send.at[kind, source],
                    out_recv.at[kind, source], (source, col),
                ).wait_recv()

            @pl.when(k < experts)
            def _():
                for level in range(len(bits)):
                    hop(kind, level, 0, col, source).start()

            for level in range(1, len(bits)):
                late = lax.rem(me - k + level + 2 * experts, experts)

                @pl.when((k >= level) & (k < experts + level))
                def _(level=level, late=late):
                    size = len(held[level - 1])
                    for slot in range(size):
                        hop_arrival(kind, level - 1, slot, late).wait_recv()
                    for later in range(level, len(bits)):
                        for slot in range(size, 2 * size):
                            hop(kind, later, slot, held[level][slot], late).start()

            return carry

        lax.fori_loop(0, experts + len(bits) - 1, advance, 0)

    for kind in range(2):

        def finish(k, carry, kind=kind):
            source = lax.rem(me + k, experts)
            last = len(bits) - 1
            for slot in range(len(held[last])):
                hop_arrival(kind, last, slot, source).wait_recv()
            for level in range(len(bits)):
                for slot in range(len(held[level])):
                    hop(kind, level, slot, held[level][slot], source).wait_send()

            @pl.when(k > 0)
            def _():
                out_copy(kind, source).wait_send()

            return carry

        lax.fori_loop(0, experts, finish, 0)


def dispatch(rows_send, cot_send, experts, parts):
    _, capacity, width = rows_send.shape
    hops = parts - 1
    full = jax.ShapeDtypeStruct((experts, capacity, width * parts), jnp.bfloat16)
    return pl.pallas_call(
        functools.partial(dispatch_kernel, experts, parts),
        out_shape=(full, full),
        in_specs=[pl.BlockSpec(memory_space=VMEM)] * 2,
        out_specs=[pl.BlockSpec(memory_space=VMEM)] * 2,
        scratch_shapes=[pltpu.SemaphoreType.DMA((2, experts))] * 2
        + [pltpu.SemaphoreType.DMA((2, hops, experts))] * 2
        + [pltpu.SemaphoreType.DMA((2,))],
        compiler_params=pltpu.CompilerParams(collective_id=0, has_side_effects=True),
        name="dispatch",
    )(rows_send, cot_send)


def column_of(row, rows):
    return jnp.broadcast_to(row, (128, rows)).T[:, 0:1]


def combine_kernel(
    experts, parts, partial_ref, conv_out_ref, mean_ref, rstd_ref, gain_ref, routed_ref, near_ref,
    *rest,
):
    bits = bits_of(parts)
    levels = len(bits)
    recv_bufs = rest[:levels]
    work, final = rest[levels], rest[levels + 1]
    hop_send, hop_recv, out_send, out_recv, sw_send, sw_recv = rest[levels + 2 :]
    me, col = lax.axis_index("sp"), lax.axis_index("tp")
    width = routed_ref.shape[2]
    greet(
        [(lax.rem(me + k, experts), col) for k in range(1, experts)]
        + [(me, flipped(col, bit)) for bit in bits]
    )
    tokens = conv_out_ref.shape[0]

    kept = [[col]]
    for bit in reversed(bits):
        kept.insert(0, kept[0] + [flipped(column, bit) for column in kept[0]])
    starts, total = [], 0
    for level in range(levels):
        starts.append(total)
        total += len(kept[level + 1])

    def columns(column):
        return pl.ds(pl.multiple_of(column * width, width), width)

    def hop(level, slot, block):
        column = flipped(kept[level + 1][slot], bits[level])
        index = starts[level] + slot
        if level == 0:
            src = partial_ref.at[block, :, columns(column)]
        else:
            src = work.at[level - 1, slot, block]
        return remote(
            src, recv_bufs[level].at[slot, block], hop_send.at[index, block],
            hop_recv.at[index, block], (me, flipped(col, bits[level])),
        )

    def summed(level, slot_column, slot_path, block):
        value = partial_ref[block, :, columns(slot_column)].astype(jnp.float32)
        for stage in range(level):
            value = value + recv_bufs[stage][slot_path[stage], block].astype(jnp.float32)
        return value

    def block_of(k):
        return lax.rem(me + k, experts)

    def start_first(k, carry):
        for slot in range(len(kept[1])):
            hop(0, slot, block_of(k)).start()
        return carry

    lax.fori_loop(1, experts + 1, start_first, 0)

    scaled = (
        (conv_out_ref[...].astype(jnp.float32) - column_of(mean_ref[...], tokens))
        * column_of(rstd_ref[...], tokens)
        * gain_ref[...]
    )
    near_ref[me // 2] = (scaled * jax.nn.sigmoid(scaled)).astype(jnp.bfloat16)

    far_bits = bits_of(experts)[:0:-1]
    sources = [[me]]
    for bit in far_bits:
        sources.append(sources[-1] + [flipped(source, bit) for source in sources[-1]])

    def sw_copy(level, slot, source):
        index = (1 << level) - 1 + slot
        return remote(
            near_ref.at[source // 2], near_ref.at[source // 2], sw_send.at[index],
            sw_recv.at[index], (flipped(me, far_bits[level]), col),
        )

    def sw_start(level):
        for slot, source in enumerate(sources[level]):
            sw_copy(level, slot, source).start()

    def sw_arrive(level):
        for slot, source in enumerate(sources[level]):
            sw_copy(level, slot, flipped(source, far_bits[level])).wait_recv()

    for level in range(1, levels):

        def middle(k, carry, level=level):
            block = block_of(k)
            for slot in range(len(kept[level])):
                hop(level - 1, slot, block).wait_recv()
            size = len(kept[level + 1])
            for slot in range(size):
                value = summed(
                    level, kept[level][size + slot], [size + slot] * level, block
                )
                work[level - 1, slot, block] = value.astype(jnp.bfloat16)
            for slot in range(size):
                hop(level, slot, block).start()
            return carry

        lax.fori_loop(1, experts + 1, middle, 0)

    sw_start(0)

    def out_copy(block):
        return remote(
            final.at[block], routed_ref.at[me], out_send.at[block], out_recv.at[me], (block, col)
        )

    def last(k, carry):
        block = block_of(k)
        hop(levels - 1, 0, block).wait_recv()
        value = summed(levels, col, [0] * levels, block).astype(jnp.bfloat16)

        @pl.when(k < experts)
        def _():
            final[block] = value
            out_copy(block).start()

        @pl.when(k == experts)
        def _():
            routed_ref[me] = value

        return carry

    lax.fori_loop(1, experts + 1, last, 0)
    for level in range(len(far_bits)):
        sw_arrive(level)
        if level + 1 < len(far_bits):
            sw_start(level + 1)

    def finish(k, carry):
        block = block_of(k)
        for level in range(levels):
            for slot in range(len(kept[level + 1])):
                hop(level, slot, block).wait_send()

        @pl.when(k < experts)
        def _():
            out_copy(block).wait_send()
            remote(
                final.at[block], routed_ref.at[block], out_send.at[block],
                out_recv.at[block], (block, col),
            ).wait_recv()

        return carry

    lax.fori_loop(1, experts + 1, finish, 0)
    for level in range(len(far_bits)):
        for slot, source in enumerate(sources[level]):
            sw_copy(level, slot, source).wait_send()


def combine(partial, conv_out, mean, rstd, gain, experts, parts):
    _, capacity, full = partial.shape
    width = full // parts
    levels = len(bits_of(parts))
    hops = parts - 1
    recv = [
        VMEM((parts >> (level + 1), experts, capacity, width), jnp.bfloat16)
        for level in range(levels)
    ]
    return pl.pallas_call(
        functools.partial(combine_kernel, experts, parts),
        out_shape=(
            jax.ShapeDtypeStruct((experts, capacity, width), jnp.bfloat16),
            jax.ShapeDtypeStruct((experts // 2,) + conv_out.shape, jnp.bfloat16),
        ),
        in_specs=[pl.BlockSpec(memory_space=VMEM)] * 5,
        out_specs=[pl.BlockSpec(memory_space=VMEM)] * 2,
        scratch_shapes=recv
        + [
            VMEM((max(levels - 1, 1), max(parts // 4, 1), experts, capacity, width), jnp.bfloat16),
            VMEM((experts, capacity, width), jnp.bfloat16),
            pltpu.SemaphoreType.DMA((hops, experts)),
            pltpu.SemaphoreType.DMA((hops, experts)),
            pltpu.SemaphoreType.DMA((experts,)),
            pltpu.SemaphoreType.DMA((experts,)),
            pltpu.SemaphoreType.DMA((experts // 2,)),
            pltpu.SemaphoreType.DMA((experts // 2,)),
        ],
        compiler_params=pltpu.CompilerParams(collective_id=1, has_side_effects=True),
        name="combine",
    )(partial, conv_out, mean, rstd, gain)


def tail_kernel(
    experts, parts, stream_ref, conv_out_ref, mean_ref, rstd_ref, gain_ref, taps_ref, proj_ref,
    near_ref, conv_ref, proj_grad_ref,
    whole, arrived, far, extended, stats, grads, norms,
    hop_send, hop_recv, out_send, out_recv, stat_send, stat_recv, halo_sem, local_sem, far_sem,
):
    me, col = lax.axis_index("sp"), lax.axis_index("tp")
    width, rows = stream_ref.shape
    full = width * parts
    block = full // experts
    bits = bits_of(parts)[::-1]
    tap_count = taps_ref.shape[0]
    halo = extended.shape[0] - rows
    greet(
        [(lax.rem(me + k, experts), col) for k in range(1, experts)]
        + [(me, lax.rem(col + k, parts)) for k in range(1, parts)]
    )

    far_copy = remote(near_ref, far, far_sem.at[0], far_sem.at[1], (flipped(me, 1), col))
    far_copy.start()

    def part(column):
        return whole.at[pl.ds(pl.multiple_of(column * width, width), width), :]

    own = pltpu.make_async_copy(stream_ref, part(col), local_sem.at[0])
    own.start()
    index, held, copies = 0, [col], []
    for level, bit in enumerate(bits):
        for slot, column in enumerate(held):
            src = stream_ref if column is col else part(column)
            copy = remote(
                src, part(column), hop_send.at[index + slot], hop_recv.at[index + slot],
                (me, flipped(col, bit)),
            )
            copy.start()
            copies.append(copy)
        for slot in range(len(held)):
            column = flipped(held[slot], bit)
            remote(
                part(column), part(column), hop_send.at[index + slot], hop_recv.at[index + slot],
                (me, flipped(col, bit)),
            ).wait_recv()
        index += len(held)
        held = held + [flipped(column, bit) for column in held]
    own.wait()

    def piece(peer):
        return whole.at[pl.ds(pl.multiple_of(peer * block, block), block), :]

    def landing(receiver, source):
        slot = lax.rem(receiver + source, 2) * (experts // 2) + source // 2
        return arrived.at[:, pl.ds(pl.multiple_of(slot * rows, rows), rows)]

    def out_copy(peer):
        return remote(piece(peer), landing(peer, me), out_send.at[peer], out_recv.at[me], (peer, col))

    def start_out(k, carry):
        out_copy(lax.rem(me + k, experts)).start()
        return carry

    lax.fori_loop(1, experts, start_out, 0)
    mine = pltpu.make_async_copy(piece(me), landing(me, me), local_sem.at[1])
    mine.start()

    gain = gain_ref[...]
    rstd = column_of(rstd_ref[...], rows)
    swished_grad = lax.dot_general(
        whole[...], proj_ref[...], OUTER_DIMS, preferred_element_type=jnp.float32
    )
    normed = (conv_out_ref[...].astype(jnp.float32) - column_of(mean_ref[...], rows)) * rstd
    scaled = normed * gain
    sig = jax.nn.sigmoid(scaled)
    scaled_grad = swished_grad * sig * (1.0 + scaled * (1.0 - sig)) * gain
    grads[...] = scaled_grad
    norms[...] = normed
    first = jnp.sum(scaled_grad, axis=1, keepdims=True)
    second = jnp.sum(scaled_grad * normed, axis=1, keepdims=True)
    lane = lax.broadcasted_iota(jnp.int32, (rows, 128), 1)
    both = jnp.where(lane == 0, first, second)
    stats[parts] = both.T[:8]
    stat_copies = []
    for k in range(1, parts):
        copy = remote(
            stats.at[parts], stats.at[k], stat_send.at[k], stat_recv.at[k],
            (me, lax.rem(col + k, parts)),
        )
        copy.start()
        stat_copies.append(copy)
    for copy in stat_copies:
        copy.wait()
    total = stats[parts]
    for k in range(1, parts):
        total = total + stats[k]
    total = total / full
    spread = jnp.concatenate([total] * 16, axis=0).T
    first_mean = spread[:, 0:1]
    second_mean = spread[:, 1:2]
    extended[0:rows, :] = rstd * (grads[...] - first_mean - norms[...] * second_mean)

    def halo_copy(device):
        return remote(
            extended.at[pl.ds(0, halo), :], extended.at[pl.ds(rows, halo), :],
            halo_sem.at[0], halo_sem.at[1], (device, col),
        )

    @pl.when(me > 0)
    def _():
        halo_copy(lax.rem(me + experts - 1, experts)).start()

    @pl.when(me == experts - 1)
    def _():
        extended[rows:, :] = jnp.zeros((halo, width), jnp.float32)

    @pl.when(me < experts - 1)
    def _():
        halo_copy(lax.rem(me + experts - 1, experts)).wait_recv()

    for start in range(0, width, 128):
        cols = pl.ds(start, 128)
        total = jnp.zeros((rows, 128), jnp.float32)
        for offset in range(tap_count):
            total = total + taps_ref[offset : offset + 1, cols] * extended[pl.ds(offset, rows), cols]
        conv_ref[:, cols] = total.astype(jnp.bfloat16)

    def finish(k, carry):
        source = lax.rem(me - k + experts, experts)
        remote(
            piece(source), landing(me, source), out_send.at[source], out_recv.at[source], (source, col)
        ).wait_recv()
        out_copy(source).wait_send()
        return carry

    lax.fori_loop(1, experts, finish, 0)
    mine.wait()
    half = experts // 2 * rows
    proj_grad_ref[...] = jnp.dot(
        arrived[:, :half], near_ref[...].reshape(half, width), preferred_element_type=jnp.float32
    )
    far_copy.wait()
    proj_grad_ref[...] += jnp.dot(
        arrived[:, half:], far[...].reshape(half, width), preferred_element_type=jnp.float32
    )
    for copy in copies:
        copy.wait_send()

    @pl.when(me > 0)
    def _():
        halo_copy(lax.rem(me + experts - 1, experts)).wait_send()


def tail(stream_t, conv_out, mean, rstd, gain, taps, proj, near, experts, parts):
    width, rows = stream_t.shape
    full = width * parts
    block = full // experts
    halo = -(-(taps.shape[0] - 1) // 8) * 8
    return pl.pallas_call(
        functools.partial(tail_kernel, experts, parts),
        out_shape=(
            jax.ShapeDtypeStruct((rows, width), jnp.bfloat16),
            jax.ShapeDtypeStruct((block, width), jnp.float32),
        ),
        in_specs=[pl.BlockSpec(memory_space=VMEM)] * 8,
        out_specs=[pl.BlockSpec(memory_space=VMEM)] * 2,
        scratch_shapes=[
            VMEM((full, rows), jnp.bfloat16),
            VMEM((block, experts * rows), jnp.bfloat16),
            VMEM(near.shape, jnp.bfloat16),
            VMEM((rows + halo, width), jnp.float32),
            VMEM((parts + 1, 8, rows), jnp.float32),
            VMEM((rows, width), jnp.float32),
            VMEM((rows, width), jnp.float32),
            pltpu.SemaphoreType.DMA((parts - 1,)),
            pltpu.SemaphoreType.DMA((parts - 1,)),
            pltpu.SemaphoreType.DMA((experts,)),
            pltpu.SemaphoreType.DMA((experts,)),
            pltpu.SemaphoreType.DMA((parts,)),
            pltpu.SemaphoreType.DMA((parts,)),
            pltpu.SemaphoreType.DMA((2,)),
            pltpu.SemaphoreType.DMA((2,)),
            pltpu.SemaphoreType.DMA((2,)),
        ],
        compiler_params=pltpu.CompilerParams(collective_id=2, has_side_effects=True),
        name="tail",
    )(stream_t, conv_out, mean, rstd, gain, taps, proj, near)


def body(
    out_cotangent,
    expert_input,
    routes,
    route_weights,
    gate_proj,
    up_proj,
    down_proj,
    conv_out,
    conv_mean,
    conv_rstd,
    norm_gain,
    taps,
    out_proj,
):
    tok_rows, local_width = out_cotangent.shape
    experts = lax.axis_size("sp")
    parts = lax.axis_size("tp")
    capacity = 3 * tok_rows // experts
    full_width = local_width * parts
    slots = experts * capacity

    chosen = routes[:, :, None] == jnp.arange(experts, dtype=jnp.int32)[None, None, :]
    named = jnp.any(chosen, axis=1)
    weight = jnp.sum(jnp.where(chosen, route_weights[:, :, None], 0.0), axis=1)
    before = jnp.arange(tok_rows)[None, :] < jnp.arange(tok_rows)[:, None]
    rank = jnp.dot(
        before.astype(jnp.bfloat16), named.astype(jnp.bfloat16), preferred_element_type=jnp.float32
    ).astype(jnp.int32)
    rank = jnp.where(named, rank, -1)
    pick = rank.T[:, None, :] == jnp.arange(capacity, dtype=jnp.int32)[None, :, None]
    slot_weight = jnp.sum(jnp.where(pick, weight.T[:, None, :], 0.0), axis=2)
    pick = pick.astype(jnp.bfloat16).reshape(slots, tok_rows)
    send_rows = jnp.dot(pick, expert_input, preferred_element_type=jnp.float32).astype(jnp.bfloat16)
    send_cot = (
        jnp.dot(pick, out_cotangent, preferred_element_type=jnp.float32)
        * slot_weight.reshape(slots, 1)
    ).astype(jnp.bfloat16)
    arrived_rows, arrived_cot = dispatch(
        send_rows.reshape(experts, capacity, local_width),
        send_cot.reshape(experts, capacity, local_width),
        experts, parts,
    )
    rows_in = arrived_rows.reshape(slots, full_width)
    cot_in = arrived_cot.reshape(slots, full_width)
    mean, rstd, gain = conv_mean[None, :], conv_rstd[None, :], norm_gain[None, :]
    gate_local = gate_proj[0]
    up_local = up_proj[0]
    down_local = down_proj[0]
    gate_pre = jnp.dot(rows_in, gate_local, preferred_element_type=jnp.float32)
    up_pre = jnp.dot(rows_in, up_local, preferred_element_type=jnp.float32)
    gate_sigmoid = jax.nn.sigmoid(gate_pre)
    activation = (gate_pre * gate_sigmoid * up_pre).astype(jnp.bfloat16)
    act_grad = lax.dot_general(cot_in, down_local, INNER_DIMS, preferred_element_type=jnp.float32)
    gate_back = (act_grad * up_pre * gate_sigmoid * (1.0 + gate_pre * (1.0 - gate_sigmoid))).astype(
        jnp.bfloat16
    )
    up_back = (act_grad * gate_pre * gate_sigmoid).astype(jnp.bfloat16)
    down_grad = lax.dot_general(
        activation, cot_in, OUTER_DIMS, preferred_element_type=jnp.float32
    ).astype(jnp.bfloat16)[None]
    gate_grad = lax.dot_general(
        rows_in, gate_back, OUTER_DIMS, preferred_element_type=jnp.float32
    ).astype(jnp.bfloat16)[None]
    up_grad = lax.dot_general(
        rows_in, up_back, OUTER_DIMS, preferred_element_type=jnp.float32
    ).astype(jnp.bfloat16)[None]
    partial_rows = lax.dot_general(
        gate_back, gate_local, INNER_DIMS, preferred_element_type=jnp.float32
    )
    partial_rows = partial_rows + lax.dot_general(
        up_back, up_local, INNER_DIMS, preferred_element_type=jnp.float32
    )
    partial = partial_rows.astype(jnp.bfloat16).reshape(experts, capacity, full_width)
    routed, near = combine(partial, conv_out, mean, rstd, gain, experts, parts)
    routed = routed.reshape(slots, local_width)
    routed_sum = lax.dot_general(pick, routed, OUTER_DIMS, preferred_element_type=jnp.float32)
    stream = (out_cotangent.astype(jnp.float32) + routed_sum).astype(jnp.bfloat16)
    conv_in_grad, proj_grad = tail(
        stream.T, conv_out, mean, rstd, gain, taps, out_proj, near, experts, parts
    )
    return (gate_grad, up_grad, down_grad, proj_grad, stream, conv_in_grad)


def solution(mesh):
    in_specs = (
        P("sp", "tp"),
        P("sp", "tp"),
        P("sp", None),
        P("sp", None),
        P("sp", None, "tp"),
        P("sp", None, "tp"),
        P("sp", "tp", None),
        P("sp", "tp"),
        P("sp"),
        P("sp"),
        P("tp"),
        P(None, "tp"),
        P(None, "tp"),
    )
    out_specs = (
        P("sp", None, "tp"),
        P("sp", None, "tp"),
        P("sp", "tp", None),
        P("sp", "tp"),
        P("sp", "tp"),
        P("sp", "tp"),
    )
    return jax.shard_map(body, mesh=mesh, in_specs=in_specs, out_specs=out_specs, check_vma=False)
```
